1024 devices in a mesh: sp: 16 (over z), dp: 64 (over y, x, core).
Axes of the slice: x: 4, y: 8, z: 16, core: 2. Of those that a mesh axis runs over, the one named last changes fastest.
Arguments:
- queries: bfloat16 [64, 2048, 1024], P('dp', 'sp'), may hold values from -300 to 300
- keys: bfloat16 [64, 2048, 1024], P('dp', 'sp'), may hold values from -7 to 7
- values: bfloat16 [64, 2048, 1024], P('dp', 'sp'), may hold values from -6 to 6
- cum_gates: float32 [64, 16, 2048], P('dp', 'sp'), may hold values from -259 to 0, as said below
- out_weight: bfloat16 [1024, 2048], P(None, 'dp'), may hold values from -0.1875 to 0.1875
Outputs:
- mixed: bfloat16 [64, 2048, 2048], P('dp', 'sp')
The draws below stay inside these ranges and needn't reach their ends.
Inputs may be any that keep to these rules, and one draw needn't show every extreme that they name: `cum_gates`: never rises along positions.
All inputs are finite; a program needn't handle non-finite values.
Results may differ from the reference program's by a relative error of at most 0.011.
Values may be sent and summed in bfloat16 or wider, within the bound.
No kernel may reach another device: no remote copies, remote signals or barrier semaphores. Data moves between devices by JAX's collectives and lax.ppermute only.
A program may use at most 64 MiB of HBM per device.

```python
import jax
import jax.numpy as jnp
from jax import lax

D = 2048
HEAD_TOTAL = 16
HEAD_DIM = 64
TOK_DEV = 128
SEQUENCE_LENGTH = 2048
SEQUENCE_COUNT = 64


def make_pair(key):
    width = HEAD_TOTAL * HEAD_DIM
    queries = jnp.clip(jax.random.normal(jax.random.fold_in(key, 11), (SEQUENCE_COUNT, SEQUENCE_LENGTH, width), jnp.float32), -6.0, 6.0)
    keys = jnp.clip(jax.random.normal(jax.random.fold_in(key, 12), (SEQUENCE_COUNT, SEQUENCE_LENGTH, width), jnp.float32), -6.0, 6.0)
    return (queries, keys)


def draw_queries(key, part):
    return make_pair(key)[0].astype(jnp.bfloat16)


def draw_keys(key, part):
    return make_pair(key)[1].astype(jnp.bfloat16)


def draw_cum_gates(key, part):
    token_position = jnp.arange(SEQUENCE_LENGTH)
    order = jax.random.permutation(jax.random.fold_in(key, 21), HEAD_TOTAL)
    slow_mask = jnp.broadcast_to((order < HEAD_TOTAL // 2)[None, :, None], (SEQUENCE_COUNT, HEAD_TOTAL, 1))
    slow_rate = jax.random.uniform(jax.random.fold_in(key, 22), (SEQUENCE_COUNT, HEAD_TOTAL, 1), jnp.float32, 0.3, 1.0) / SEQUENCE_LENGTH
    fast_rate = jnp.exp(jax.random.uniform(jax.random.fold_in(key, 23), (SEQUENCE_COUNT, HEAD_TOTAL, 1), jnp.float32, jnp.log(1.0 / 100.0), jnp.log(1.0 / 30.0)))
    rate = jnp.where(slow_mask, slow_rate, fast_rate)
    block_count = SEQUENCE_LENGTH // TOK_DEV
    block_factor = jnp.exp(jax.random.uniform(jax.random.fold_in(key, 24), (SEQUENCE_COUNT, 1, block_count), jnp.float32, jnp.log(0.5), jnp.log(2.0)))
    factor = block_factor[:, :, token_position // TOK_DEV]
    rough = jax.random.uniform(jax.random.fold_in(key, 25), (SEQUENCE_COUNT, HEAD_TOTAL, SEQUENCE_LENGTH), jnp.float32, 0.3, 1.7)
    logarithm_gate = -rate * factor * rough
    spike_location = jax.random.randint(jax.random.fold_in(key, 26), (SEQUENCE_COUNT, HEAD_TOTAL, 3), 0, SEQUENCE_LENGTH)
    spike_decrease = jax.random.uniform(jax.random.fold_in(key, 27), (SEQUENCE_COUNT, HEAD_TOTAL, 3), jnp.float32, 0.2, 0.5)
    match_count = (token_position[None, None, None, :] == spike_location[:, :, :, None]).astype(jnp.float32)
    spike_events = jnp.sum(match_count * jnp.log(1.0 - spike_decrease)[:, :, :, None], axis=2)
    return jnp.cumsum(logarithm_gate + spike_events, axis=-1).astype(jnp.float32)


def level_of(rng, extent, pieces, smallest, largest):
    loudness = 1.0
    for position, parts in pieces:
        draws = jax.random.uniform(jax.random.fold_in(jax.random.fold_in(rng, 6), position), (parts,), jnp.float32, smallest / len(pieces), largest / len(pieces))
        loudness = loudness * jnp.repeat(jnp.exp(draws), extent[position] // parts).reshape((-1,) + (1,) * (len(extent) - 1 - position))
    return loudness


def gaussian(rng, dims, spread, limit, split=(), dtype=jnp.bfloat16):
    entries = spread * jax.random.normal(rng, dims, jnp.float32)
    if split:
        entries = entries * level_of(rng, dims, split, -0.22, 0.18)
    return jnp.clip(entries, -limit, limit).astype(dtype)


def setup_inputs(seed: int = 0) -> dict:
    arg_keys = jax.random.split(jax.random.key(seed), 6)
    return {
        "queries": draw_queries(jax.random.fold_in(arg_keys[5], 71), 0),
        "keys": draw_keys(jax.random.fold_in(arg_keys[5], 71), 0),
        "values": gaussian(arg_keys[2], (SEQUENCE_COUNT, SEQUENCE_LENGTH, HEAD_TOTAL * HEAD_DIM), 1.0, 6.0, ((0, 64), (1, 16))),
        "cum_gates": draw_cum_gates(jax.random.fold_in(arg_keys[5], 71), 0),
        "out_weight": gaussian(arg_keys[4], (HEAD_TOTAL * HEAD_DIM, D), (HEAD_TOTAL * HEAD_DIM) ** -0.5, 0.1875, ((1, 64),)),
    }


def attend_sequence(packed, out_weight):
    query_rows, key_rows, value_rows, cum_rows = packed
    length = query_rows.shape[0]
    head_count = cum_rows.shape[0]
    head_size = query_rows.shape[1] // head_count
    query_heads = query_rows.astype(jnp.float32).reshape(length, head_count, head_size).transpose(1, 0, 2)
    key_heads = key_rows.astype(jnp.float32).reshape(length, head_count, head_size).transpose(1, 0, 2)
    value_heads = value_rows.astype(jnp.float32).reshape(length, head_count, head_size).transpose(1, 0, 2)
    scores = jnp.einsum('hqd,hkd->hqk', query_heads, key_heads) * (head_size ** -0.5)
    scores = scores + cum_rows[:, :, None] - cum_rows[:, None, :]
    token_position = jnp.arange(length)
    scores = jnp.where(token_position[None, :] <= token_position[:, None], scores, -jnp.inf)
    row_max = jnp.max(scores, axis=-1, keepdims=True)
    expon = jnp.exp(scores - row_max)
    weights = (expon / jnp.sum(expon, axis=-1, keepdims=True)).astype(jnp.bfloat16)
    head_out = jnp.einsum('hqk,hkd->hqd', weights.astype(jnp.float32), value_heads).astype(jnp.bfloat16)
    head_out = head_out.transpose(1, 0, 2).reshape(length, head_count * head_size)
    return jnp.dot(head_out, out_weight, preferred_element_type=jnp.float32).astype(jnp.bfloat16)


def reference(queries, keys, values, cum_gates, out_weight):
    return lax.map(lambda packed: attend_sequence(packed, out_weight), (queries, keys, values, cum_gates))
```

```python
import jax
import jax.numpy as jnp
from jax import lax
from jax.experimental import pallas as pl
from jax.experimental.pallas import tpu as pltpu
from jax.sharding import Mesh
from jax.sharding import PartitionSpec as P


DP = ("dp_0", "dp_1", "dp_2")
VMEM = pl.BlockSpec(memory_space=pltpu.VMEM)
SMEM = pl.BlockSpec(memory_space=pltpu.SMEM)


def pack_kernel(q_hbm, k_hbm, v_hbm, out_ref, q_ref, k_ref, v_ref, sems):
    rows, width = q_ref.shape
    half = 64
    copies = [
        pltpu.make_async_copy(src.at[0], dst, sems.at[n])
        for n, (src, dst) in enumerate(((k_hbm, k_ref), (v_hbm, v_ref), (q_hbm, q_ref)))
    ]
    for copy in copies:
        copy.start()
    copies[0].wait()
    for j in range(width // 128):
        turned = k_ref[:, j * 128 : (j + 1) * 128].T
        out_ref[2 * j, rows:, :] = turned[:half]
        out_ref[2 * j + 1, rows:, :] = turned[half:]
    copies[1].wait()
    copies[2].wait()
    for j in range(width // 128):
        cols = slice(j * 128, (j + 1) * 128)
        q, v = q_ref[:, cols] * jnp.bfloat16(0.125), v_ref[:, cols]
        out_ref[2 * j, 0:rows, :] = jnp.concatenate([v[:, :half], q[:, :half]], axis=1)
        out_ref[2 * j + 1, 0:rows, :] = jnp.concatenate([v[:, half:], q[:, half:]], axis=1)


def pack(queries, keys, values):
    return pl.pallas_call(
        pack_kernel,
        out_shape=pltpu.VMEM((16, 192, 128), jnp.bfloat16),
        in_specs=[pl.BlockSpec(memory_space=pltpu.HBM)] * 3,
        out_specs=VMEM,
        scratch_shapes=[pltpu.VMEM((128, 1024), jnp.bfloat16)] * 3 + [pltpu.SemaphoreType.DMA((3,))],
    )(queries, keys, values)


def attend_kernel(x_ref, cum_ref, out_ref, keys_ref, vals_ref):
    blocks = x_ref.shape[0]
    length = blocks * 128
    keys_ref[0:64, :] = jnp.zeros((64, length), jnp.bfloat16)
    vals_ref[:, 128:] = jnp.ones((length, 128), jnp.bfloat16)
    for p in range(blocks):
        keys_ref[64:128, p * 128 : (p + 1) * 128] = x_ref[p, 128:192, :]
        vals_ref[p * 128 : (p + 1) * 128, 0:128] = x_ref[p, 0:128, :]
    step = 256
    row = lax.broadcasted_iota(jnp.int32, (step, step), 0)
    col = lax.broadcasted_iota(jnp.int32, (step, step), 1)
    for i in range(length // step):
        here, upto = slice(i * step, (i + 1) * step), (i + 1) * step
        scores = jnp.dot(
            vals_ref[here, 0:128], keys_ref[:, :upto], preferred_element_type=jnp.float32
        )
        scores = scores - cum_ref[:, :upto]
        last = jnp.where(col <= row, scores[:, upto - step :], -jnp.inf)
        scores = jnp.concatenate([scores[:, : upto - step], last], axis=1) if i else last
        top = jnp.max(scores, axis=1, keepdims=True)
        expon = jnp.exp(scores - top).astype(jnp.bfloat16)
        both = jnp.dot(expon, vals_ref[:upto, :], preferred_element_type=jnp.float32)
        head = (both[:, :128] / both[:, 128:]).astype(jnp.bfloat16).T
        out_ref[2 * i] = head[0:64, 0:128]
        out_ref[2 * i + 1] = head[0:64, 128:256]


def attend(packed, cum):
    length = cum.shape[1]
    return pl.pallas_call(
        attend_kernel,
        out_shape=pltpu.VMEM((16, 64, 128), jnp.bfloat16),
        in_specs=[VMEM] * 2,
        out_specs=VMEM,
        scratch_shapes=[
            pltpu.VMEM((128, length), jnp.bfloat16),
            pltpu.VMEM((length, 256), jnp.bfloat16),
        ],
        compiler_params=pltpu.CompilerParams(vmem_limit_bytes=28 << 20),
    )(packed, cum)


def project_kernel(base_ref, head_ref, *refs):
    *parts, out_ref, turned_ref = refs
    heads = head_ref[...]
    for n, part in enumerate(parts):
        rows = jnp.dot(part[...], heads, preferred_element_type=jnp.float32)
        for y in range(8):
            place = pl.multiple_of(base_ref[n] + base_ref[len(parts) + y], 32)
            turned_ref[pl.ds(place, 32), :] = rows[y * 32 : (y + 1) * 32]
    for n in range(out_ref.shape[1] // 128):
        cols = slice(n * 128, (n + 1) * 128)
        out_ref[:, cols] = turned_ref[cols, :].astype(jnp.bfloat16).T


def project(heads, parts, bases):
    return pl.pallas_call(
        project_kernel,
        out_shape=jax.ShapeDtypeStruct((128, 2048), jnp.bfloat16),
        in_specs=[SMEM] + [VMEM] * (1 + len(parts)),
        out_specs=VMEM,
        scratch_shapes=[pltpu.VMEM((2048, 128), jnp.float32)],
        compiler_params=pltpu.CompilerParams(vmem_limit_bytes=12 << 20),
    )(bases, heads, *parts)


def shift(value, axis, by):
    n = lax.axis_size(axis)
    return lax.ppermute(value, axis, [(s, (s + by) % n) for s in range(n)])


def gather_weight(out_weight):
    y, x, core = (lax.axis_index(axis) for axis in DP)
    rows = out_weight.T
    for by in (4, 2, 1):
        rows = jnp.concatenate([rows, shift(rows, "dp_0", by)])
    there = [(i * 2 + c, (i + 1 - 2 * c) % 4 * 2 + c) for i in range(4) for c in range(2)]
    back = [(target, source) for source, target in there]
    near = [lax.ppermute(rows, DP[1:], way) for way in (there, back)]
    far = lax.ppermute(near[0], DP[1:], there)
    pieces = [rows, *near, far]
    others = [shift(rows, "dp_2", 1)]
    others += [shift(piece, "dp_2", 1) for piece in pieces[1:]]
    cores = core ^ jnp.array([0, 0, 0, 0, 1, 1, 1, 1], jnp.int32)
    owners = (x + jnp.array([0, -1, 1, 2] * 2, jnp.int32) * (1 - 2 * cores)) & 3
    places = (y - jnp.array([0, 4, 2, 6, 1, 5, 3, 7], jnp.int32)) & 7
    return pieces + others, jnp.concatenate([(owners * 2 + cores) * 32, places * 256])


def shards(queries, keys, values, cum_gates, out_weight):
    packed = pack(queries, keys, values)
    packed = lax.all_to_all(packed, "sp", split_axis=0, concat_axis=0, tiled=True)
    parts, bases = gather_weight(out_weight)
    heads = attend(packed, cum_gates[0])
    heads = lax.all_to_all(heads, "sp", split_axis=0, concat_axis=0, tiled=True)
    return project(heads.reshape(1024, 128), parts, bases)[None]


def solution(mesh):
    split = Mesh(mesh.devices.reshape(mesh.shape["sp"], 8, 4, 2), ("sp", "dp_0", "dp_1", "dp_2"))
    placed = (
        P(DP, "sp", None),
        P(DP, "sp", None),
        P(DP, "sp", None),
        P(DP, "sp", None),
        P(None, DP),
    )
    return jax.shard_map(
        shards, mesh=split, in_specs=placed, out_specs=P(DP, "sp", None), check_vma=False
    )
```

```python
import jax
import jax.numpy as jnp
from jax import lax
from jax.experimental import pallas as pl
from jax.experimental.pallas import tpu as pltpu
from jax.sharding import Mesh
from jax.sharding import PartitionSpec as P


DP = ("dp_0", "dp_1", "dp_2")
VMEM = pl.BlockSpec(memory_space=pltpu.VMEM)
SMEM = pl.BlockSpec(memory_space=pltpu.SMEM)
HBM = pl.BlockSpec(memory_space=pltpu.HBM)
STEP, PART = 256, 128


def pack_kernel(q_hbm, k_hbm, v_hbm, out_hbm, q_ref, k_ref, v_ref, out_ref, sems):
    _, width = q_ref.shape
    half = 64
    copies = [
        pltpu.make_async_copy(src.at[0], dst, sems.at[n])
        for n, (src, dst) in enumerate(((q_hbm, q_ref), (v_hbm, v_ref), (k_hbm, k_ref)))
    ]
    for copy in copies:
        copy.start()

    def send(n):
        third = pl.ds(n * half, half)
        copies.append(
            pltpu.make_async_copy(out_ref.at[:, third], out_hbm.at[:, third], sems.at[3 + n])
        )
        copies[-1].start()

    copies[0].wait()
    for j in range(width // 128):
        turned = (q_ref[:, j * 128 : (j + 1) * 128] * jnp.bfloat16(0.125)).T
        out_ref[2 * j, 0:half, :] = turned[:half]
        out_ref[2 * j + 1, 0:half, :] = turned[half:]
    send(0)
    copies[1].wait()
    for j in range(width // 128):
        turned = v_ref[:, j * 128 : (j + 1) * 128].T
        out_ref[2 * j, half : 2 * half, :] = turned[:half]
        out_ref[2 * j + 1, half : 2 * half, :] = turned[half:]
    send(1)
    copies[2].wait()
    for j in range(width // 128):
        k = k_ref[:, j * 128 : (j + 1) * 128]
        out_ref[2 * j, 2 * half :, :] = jnp.concatenate([k[:half, :half], k[half:, :half]], axis=1)
        out_ref[2 * j + 1, 2 * half :, :] = jnp.concatenate([k[:half, half:], k[half:, half:]], axis=1)
    send(2)
    for copy in copies[3:]:
        copy.wait()


def pack(queries, keys, values):
    return pl.pallas_call(
        pack_kernel,
        out_shape=jax.ShapeDtypeStruct((16, 192, 128), jnp.bfloat16),
        in_specs=[HBM] * 3,
        out_specs=HBM,
        scratch_shapes=[pltpu.VMEM((128, 1024), jnp.bfloat16)] * 3
        + [pltpu.VMEM((16, 192, 128), jnp.bfloat16), pltpu.SemaphoreType.DMA((6,))],
    )(queries, keys, values)


def attend_kernel(x_ref, cum_ref, out_hbm, out_ref, sems, keys_ref, queries_ref, values_ref, score_ref, expon_ref):
    blocks = x_ref.shape[0]
    length = blocks * 128
    tiles = length // STEP
    lane = lax.broadcasted_iota(jnp.int32, (64, 128), 1)
    row = lax.broadcasted_iota(jnp.int32, (PART, STEP), 0)
    col = lax.broadcasted_iota(jnp.int32, (PART, STEP), 1)

    gates = -cum_ref[...]
    high = gates.astype(jnp.bfloat16).astype(jnp.float32)
    mid = (gates - high).astype(jnp.bfloat16).astype(jnp.float32)
    low = gates - high - mid
    blank = jnp.zeros((64, 128), jnp.float32)
    turned = jnp.concatenate([blank, high, mid, low, blank[:16]], axis=0).T.astype(jnp.bfloat16)
    queries_ref[64:112, :] = jnp.ones((48, length), jnp.bfloat16)
    queries_ref[112:, :] = jnp.zeros((16, length), jnp.bfloat16)
    values_ref[64:, :] = jnp.ones((16, length), jnp.bfloat16)
    nothing = jnp.zeros((64, 128), jnp.bfloat16)
    for p in range(blocks):
        spot = slice(p * 128, (p + 1) * 128)
        queries_ref[0:64, spot] = x_ref[p, 0:64, :]
        values_ref[0:64, spot] = x_ref[p, 64:128, :]
        both = x_ref[p, 128:192, :]
        other = jnp.concatenate([both[:, 64:], both[:, :64]], axis=1)
        for keys, part in ((both, 0), (other, 64)):
            gate = jnp.where((lane & 15) == p, turned[part : part + 64], nothing)
            keys_ref[p * 128 + part : p * 128 + part + 64, :] = jnp.where(lane < 64, keys, gate)

    def score(i, s, top):
        scores = jnp.dot(keys_ref[s : s + PART, :], queries_ref[:, i * STEP : (i + 1) * STEP], preferred_element_type=jnp.float32)
        if s >= i * STEP:
            scores = jnp.where(row + (s - i * STEP) <= col, scores, -jnp.inf)
        score_ref[i % 2, s : s + PART, :] = scores
        most = jnp.max(scores.reshape(PART // 8, 8, STEP), axis=0)
        return most if top is None else jnp.maximum(top, most)

    def weigh(i, s, top):
        expon_ref[i % 2, s : s + PART, :] = jnp.exp(score_ref[i % 2, s : s + PART, :] - top).astype(jnp.bfloat16)

    def finish(i):
        upto = (i + 1) * STEP
        both = jnp.dot(values_ref[:, :upto], expon_ref[i % 2, :upto, :], preferred_element_type=jnp.float32)
        head = (both[0:64] / both[64:65]).astype(jnp.bfloat16)
        out_ref[2 * i] = head[:, 0:128]
        out_ref[2 * i + 1] = head[:, 128:256]
        pair = pl.ds(2 * i, 2)
        copies.append(pltpu.make_async_copy(out_ref.at[pair], out_hbm.at[pair], sems.at[i]))
        copies[-1].start()

    copies = []
    tops = {}
    order = list(reversed(range(tiles)))
    for n, i in enumerate(order + [None]):
        before = order[n - 1] if n else None
        todo = list(range(0, (i + 1) * STEP, PART)) if i is not None else []
        late = list(range(0, (before + 1) * STEP, PART)) if n else []
        top = None
        for m in range(max(len(todo), len(late))):
            if m < len(late):
                weigh(before, late[m], tops[before])
            if m < len(todo):
                top = score(i, todo[m], top)
        if top is not None:
            tops[i] = jnp.max(top, axis=0, keepdims=True)
        if n:
            finish(before)
    for copy in copies:
        copy.wait()


def attend(packed, cum):
    length = cum.size
    return pl.pallas_call(
        attend_kernel,
        out_shape=jax.ShapeDtypeStruct((16, 64, 128), jnp.bfloat16),
        in_specs=[VMEM] * 2,
        out_specs=HBM,
        scratch_shapes=[
            pltpu.VMEM((16, 64, 128), jnp.bfloat16),
            pltpu.SemaphoreType.DMA((8,)),
            pltpu.VMEM((length, 128), jnp.bfloat16),
            pltpu.VMEM((128, length), jnp.bfloat16),
            pltpu.VMEM((80, length), jnp.bfloat16),
            pltpu.VMEM((2, length, STEP), jnp.float32),
            pltpu.VMEM((2, length, STEP), jnp.bfloat16),
        ],
        compiler_params=pltpu.CompilerParams(vmem_limit_bytes=28 << 20),
    )(packed, cum)


def project_kernel(base_ref, head_ref, *refs):
    *parts, out_ref, turned_ref = refs
    heads = head_ref[...]
    for n, part in enumerate(parts):
        rows = jnp.dot(part[...], heads, preferred_element_type=jnp.float32)
        for y in range(8):
            place = pl.multiple_of(base_ref[n] + base_ref[len(parts) + y], 32)
            turned_ref[pl.ds(place, 32), :] = rows[y * 32 : (y + 1) * 32]
    for n in range(out_ref.shape[2] // 128):
        cols = slice(n * 128, (n + 1) * 128)
        out_ref[0, :, cols] = turned_ref[cols, :].astype(jnp.bfloat16).T


def project(heads, parts, bases):
    return pl.pallas_call(
        project_kernel,
        out_shape=jax.ShapeDtypeStruct((1, 128, 2048), jnp.bfloat16),
        in_specs=[SMEM] + [VMEM] * 9,
        out_specs=VMEM,
        scratch_shapes=[pltpu.VMEM((2048, 128), jnp.float32)],
        compiler_params=pltpu.CompilerParams(vmem_limit_bytes=12 << 20),
    )(bases, heads, *parts)


def shift(value, axis, by):
    n = lax.axis_size(axis)
    return lax.ppermute(value, axis, [(s, (s + by) % n) for s in range(n)])


def gather_weight(out_weight):
    y, x, core = (lax.axis_index(axis) for axis in DP)
    rows = out_weight.T
    for by in (4, 2, 1):
        rows = jnp.concatenate([rows, shift(rows, "dp_0", by)])
    there = [(i * 2 + c, (i + 1 - 2 * c) % 4 * 2 + c) for i in range(4) for c in range(2)]
    back = [(target, source) for source, target in there]
    near = [lax.ppermute(rows, DP[1:], way) for way in (there, back)]
    far = lax.ppermute(near[0], DP[1:], there)
    pieces = [rows, *near, far]
    others = [shift(rows, "dp_2", 1)]
    others += [shift(piece, "dp_2", 1) for piece in pieces[1:]]
    cores = core ^ jnp.array([0, 0, 0, 0, 1, 1, 1, 1], jnp.int32)
    owners = (x + jnp.array([0, -1, 1, 2] * 2, jnp.int32) * (1 - 2 * cores)) & 3
    places = (y - jnp.array([0, 4, 2, 6, 1, 5, 3, 7], jnp.int32)) & 7
    return pieces + others, jnp.concatenate([(owners * 2 + cores) * 32, places * 256])


def shards(queries, keys, values, cum_gates, out_weight):
    packed = pack(queries, keys, values)
    packed = lax.all_to_all(packed, "sp", split_axis=0, concat_axis=0, tiled=True)
    parts, bases = gather_weight(out_weight)
    heads = attend(packed, cum_gates.reshape(16, 128))
    heads = lax.all_to_all(heads, "sp", split_axis=0, concat_axis=0, tiled=True)
    return project(heads.reshape(1024, 128), parts, bases)


def solution(mesh):
    split = Mesh(mesh.devices.reshape(mesh.shape["sp"], 8, 4, 2), ("sp", "dp_0", "dp_1", "dp_2"))
    placed = (
        P(DP, "sp", None),
        P(DP, "sp", None),
        P(DP, "sp", None),
        P(DP, "sp", None),
        P(None, DP),
    )
    return jax.shard_map(
        shards, mesh=split, in_specs=placed, out_specs=P(DP, "sp", None), check_vma=False
    )
```

```python
import jax
import jax.numpy as jnp
from jax import lax
from jax.experimental import pallas as pl
from jax.experimental.pallas import tpu as pltpu
from jax.sharding import Mesh
from jax.sharding import PartitionSpec as P


DP = ("dp_0", "dp_1", "dp_2")
VMEM = pl.BlockSpec(memory_space=pltpu.VMEM)
HBM = pl.BlockSpec(memory_space=pltpu.HBM)
STEP, PART = 256, 128


def pack_kernel(q_hbm, k_hbm, v_hbm, out_hbm, q_ref, k_ref, v_ref, out_ref, sems):
    _, width = q_ref.shape
    half = 64
    copies = [
        pltpu.make_async_copy(src.at[0], dst, sems.at[n])
        for n, (src, dst) in enumerate(((q_hbm, q_ref), (v_hbm, v_ref), (k_hbm, k_ref)))
    ]
    for copy in copies:
        copy.start()

    def send(n):
        third = pl.ds(n * half, half)
        copies.append(
            pltpu.make_async_copy(out_ref.at[:, third], out_hbm.at[:, third], sems.at[3 + n])
        )
        copies[-1].start()

    copies[0].wait()
    for j in range(width // 128):
        turned = (q_ref[:, j * 128 : (j + 1) * 128] * jnp.bfloat16(0.125)).T
        out_ref[2 * j, 0:half, :] = turned[:half]
        out_ref[2 * j + 1, 0:half, :] = turned[half:]
    send(0)
    copies[1].wait()
    for j in range(width // 128):
        turned = v_ref[:, j * 128 : (j + 1) * 128].T
        out_ref[2 * j, half : 2 * half, :] = turned[:half]
        out_ref[2 * j + 1, half : 2 * half, :] = turned[half:]
    send(1)
    copies[2].wait()
    for j in range(width // 128):
        k = k_ref[:, j * 128 : (j + 1) * 128]
        out_ref[2 * j, 2 * half :, :] = jnp.concatenate([k[:half, :half], k[half:, :half]], axis=1)
        out_ref[2 * j + 1, 2 * half :, :] = jnp.concatenate([k[:half, half:], k[half:, half:]], axis=1)
    send(2)
    for copy in copies[3:]:
        copy.wait()


def pack(queries, keys, values):
    return pl.pallas_call(
        pack_kernel,
        out_shape=jax.ShapeDtypeStruct((16, 192, 128), jnp.bfloat16),
        in_specs=[HBM] * 3,
        out_specs=HBM,
        scratch_shapes=[pltpu.VMEM((128, 1024), jnp.bfloat16)] * 3
        + [pltpu.VMEM((16, 192, 128), jnp.bfloat16), pltpu.SemaphoreType.DMA((6,))],
    )(queries, keys, values)


def attend_kernel(x_ref, cum_ref, out_hbm, out_ref, sems, keys_ref, queries_ref, values_ref, score_ref, expon_ref):
    blocks = x_ref.shape[0]
    length = blocks * 128
    tiles = length // STEP
    lane = lax.broadcasted_iota(jnp.int32, (64, 128), 1)
    row = lax.broadcasted_iota(jnp.int32, (PART, STEP), 0)
    col = lax.broadcasted_iota(jnp.int32, (PART, STEP), 1)

    gates = -cum_ref[...]
    high = gates.astype(jnp.bfloat16).astype(jnp.float32)
    mid = (gates - high).astype(jnp.bfloat16).astype(jnp.float32)
    low = gates - high - mid
    blank = jnp.zeros((64, 128), jnp.float32)
    turned = jnp.concatenate([blank, high, mid, low, blank[:16]], axis=0).T.astype(jnp.bfloat16)
    queries_ref[64:112, :] = jnp.ones((48, length), jnp.bfloat16)
    queries_ref[112:, :] = jnp.zeros((16, length), jnp.bfloat16)
    values_ref[64:, :] = jnp.ones((16, length), jnp.bfloat16)
    nothing = jnp.zeros((64, 128), jnp.bfloat16)
    for p in range(blocks):
        spot = slice(p * 128, (p + 1) * 128)
        queries_ref[0:64, spot] = x_ref[p, 0:64, :]
        values_ref[0:64, spot] = x_ref[p, 64:128, :]
        both = x_ref[p, 128:192, :]
        other = jnp.concatenate([both[:, 64:], both[:, :64]], axis=1)
        for keys, part in ((both, 0), (other, 64)):
            gate = jnp.where((lane & 15) == p, turned[part : part + 64], nothing)
            keys_ref[p * 128 + part : p * 128 + part + 64, :] = jnp.where(lane < 64, keys, gate)

    def score(i, s, top):
        scores = jnp.dot(keys_ref[s : s + PART, :], queries_ref[:, i * STEP : (i + 1) * STEP], preferred_element_type=jnp.float32)
        if s >= i * STEP:
            scores = jnp.where(row + (s - i * STEP) <= col, scores, -jnp.inf)
        score_ref[i % 2, s : s + PART, :] = scores
        most = jnp.max(scores.reshape(PART // 8, 8, STEP), axis=0)
        return most if top is None else jnp.maximum(top, most)

    def weigh(i, s, top):
        expon_ref[i % 2, s : s + PART, :] = jnp.exp(score_ref[i % 2, s : s + PART, :] - top).astype(jnp.bfloat16)

    def finish(i):
        upto = (i + 1) * STEP
        both = jnp.dot(values_ref[:, :upto], expon_ref[i % 2, :upto, :], preferred_element_type=jnp.float32)
        head = (both[0:64] / both[64:65]).astype(jnp.bfloat16)
        out_ref[2 * i] = head[:, 0:128]
        out_ref[2 * i + 1] = head[:, 128:256]
        pair = pl.ds(2 * i, 2)
        copies.append(pltpu.make_async_copy(out_ref.at[pair], out_hbm.at[pair], sems.at[i]))
        copies[-1].start()

    copies = []
    tops = {}
    order = list(reversed(range(tiles)))
    for n, i in enumerate(order + [None]):
        before = order[n - 1] if n else None
        todo = list(range(0, (i + 1) * STEP, PART)) if i is not None else []
        late = list(range(0, (before + 1) * STEP, PART)) if n else []
        top = None
        for m in range(max(len(todo), len(late))):
            if m < len(late):
                weigh(before, late[m], tops[before])
            if m < len(todo):
                top = score(i, todo[m], top)
        if top is not None:
            tops[i] = jnp.max(top, axis=0, keepdims=True)
        if n:
            finish(before)
    for copy in copies:
        copy.wait()


def attend(packed, cum):
    length = cum.size
    return pl.pallas_call(
        attend_kernel,
        out_shape=jax.ShapeDtypeStruct((16, 64, 128), jnp.bfloat16),
        in_specs=[VMEM] * 2,
        out_specs=HBM,
        scratch_shapes=[
            pltpu.VMEM((16, 64, 128), jnp.bfloat16),
            pltpu.SemaphoreType.DMA((8,)),
            pltpu.VMEM((length, 128), jnp.bfloat16),
            pltpu.VMEM((128, length), jnp.bfloat16),
            pltpu.VMEM((80, length), jnp.bfloat16),
            pltpu.VMEM((2, length, STEP), jnp.float32),
            pltpu.VMEM((2, length, STEP), jnp.bfloat16),
        ],
        compiler_params=pltpu.CompilerParams(vmem_limit_bytes=28 << 20),
    )(packed, cum)


def project_kernel(spot_ref, head_ref, *refs):
    *parts, out_ref, turned_ref = refs
    y, x, core = spot_ref[0], spot_ref[1], spot_ref[2]
    heads = head_ref[...]
    for n, part in enumerate(parts):
        owner = core if n < 4 else 1 - core
        base = (((x + (0, -1, 1, 2)[n % 4] * (1 - 2 * owner)) & 3) * 2 + owner) * 32
        rows = jnp.dot(part[...], heads, preferred_element_type=jnp.float32)
        for m, back in enumerate((0, 4, 2, 6, 1, 5, 3, 7)):
            place = pl.multiple_of(((y - back) & 7) * 256 + base, 32)
            turned_ref[pl.ds(place, 32), :] = rows[m * 32 : (m + 1) * 32]
    for n in range(out_ref.shape[2] // 128):
        cols = slice(n * 128, (n + 1) * 128)
        out_ref[0, :, cols] = turned_ref[cols, :].astype(jnp.bfloat16).T


def project(heads, parts):
    spot = jnp.stack([lax.axis_index(axis) for axis in DP])
    return pl.pallas_call(
        project_kernel,
        out_shape=jax.ShapeDtypeStruct((1, 128, 2048), jnp.bfloat16),
        in_specs=[pl.BlockSpec(memory_space=pltpu.SMEM)] + [VMEM] * (1 + len(parts)),
        out_specs=VMEM,
        scratch_shapes=[pltpu.VMEM((2048, 128), jnp.float32)],
        compiler_params=pltpu.CompilerParams(vmem_limit_bytes=12 << 20),
    )(spot, heads, *parts)


def shift(value, axis, by):
    n = lax.axis_size(axis)
    return lax.ppermute(value, axis, [(s, (s + by) % n) for s in range(n)])


def gather_weight(out_weight):
    rows = out_weight.T
    for by in (4, 2, 1):
        rows = jnp.concatenate([rows, shift(rows, "dp_0", by)])
    there = [(i * 2 + c, (i + 1 - 2 * c) % 4 * 2 + c) for i in range(4) for c in range(2)]
    back = [(target, source) for source, target in there]
    near = [lax.ppermute(rows, DP[1:], way) for way in (there, back)]
    far = lax.ppermute(near[0], DP[1:], there)
    pieces = [rows, *near, far]
    others = [shift(rows, "dp_2", 1)]
    others += [shift(piece, "dp_2", 1) for piece in pieces[1:]]
    return pieces + others


def shards(queries, keys, values, cum_gates, out_weight):
    packed = pack(queries, keys, values)
    packed = lax.all_to_all(packed, "sp", split_axis=0, concat_axis=0, tiled=True)
    parts = gather_weight(out_weight)
    heads = attend(packed, cum_gates.reshape(16, 128))
    heads = lax.all_to_all(heads, "sp", split_axis=0, concat_axis=0, tiled=True)
    return project(heads.reshape(1024, 128), parts)


def solution(mesh):
    split = Mesh(mesh.devices.reshape(mesh.shape["sp"], 8, 4, 2), ("sp", "dp_0", "dp_1", "dp_2"))
    placed = (
        P(DP, "sp", None),
        P(DP, "sp", None),
        P(DP, "sp", None),
        P(DP, "sp", None),
        P(None, DP),
    )
    return jax.shard_map(
        shards, mesh=split, in_specs=placed, out_specs=P(DP, "sp", None), check_vma=False
    )
```

```python
import jax
import jax.numpy as jnp
from jax import lax
from jax.experimental import pallas as pl
from jax.experimental.pallas import tpu as pltpu
from jax.sharding import Mesh
from jax.sharding import PartitionSpec as P


DP = ("dp_0", "dp_1", "dp_2")
VMEM = pl.BlockSpec(memory_space=pltpu.VMEM)
HBM = pl.BlockSpec(memory_space=pltpu.HBM)
STEP, PART = 256, 128


def pack_kernel(q_hbm, k_hbm, v_hbm, out_hbm, q_ref, k_ref, v_ref, out_ref, sems):
    _, width = q_ref.shape
    half = 64
    copies = [
        pltpu.make_async_copy(src.at[0], dst, sems.at[n])
        for n, (src, dst) in enumerate(((q_hbm, q_ref), (v_hbm, v_ref), (k_hbm, k_ref)))
    ]
    for copy in copies:
        copy.start()

    def send(n):
        third = pl.ds(n * half, half)
        copies.append(
            pltpu.make_async_copy(out_ref.at[:, third], out_hbm.at[:, third], sems.at[3 + n])
        )
        copies[-1].start()

    copies[0].wait()
    for j in range(width // 128):
        turned = (q_ref[:, j * 128 : (j + 1) * 128] * jnp.bfloat16(0.125)).T
        out_ref[2 * j, 0:half, :] = turned[:half]
        out_ref[2 * j + 1, 0:half, :] = turned[half:]
    send(0)
    copies[1].wait()
    for j in range(width // 128):
        turned = v_ref[:, j * 128 : (j + 1) * 128].T
        out_ref[2 * j, half : 2 * half, :] = turned[:half]
        out_ref[2 * j + 1, half : 2 * half, :] = turned[half:]
    send(1)
    copies[2].wait()
    for j in range(width // 128):
        k = k_ref[:, j * 128 : (j + 1) * 128]
        out_ref[2 * j, 2 * half :, :] = jnp.concatenate([k[:half, :half], k[half:, :half]], axis=1)
        out_ref[2 * j + 1, 2 * half :, :] = jnp.concatenate([k[:half, half:], k[half:, half:]], axis=1)
    send(2)
    for copy in copies[3:]:
        copy.wait()


def pack(queries, keys, values):
    return pl.pallas_call(
        pack_kernel,
        out_shape=jax.ShapeDtypeStruct((16, 192, 128), jnp.bfloat16),
        in_specs=[HBM] * 3,
        out_specs=HBM,
        scratch_shapes=[pltpu.VMEM((128, 1024), jnp.bfloat16)] * 3
        + [pltpu.VMEM((16, 192, 128), jnp.bfloat16), pltpu.SemaphoreType.DMA((6,))],
    )(queries, keys, values)


def attend_kernel(x_ref, cum_ref, out_hbm, out_ref, sems, keys_ref, queries_ref, values_ref, score_ref, expon_ref):
    blocks = x_ref.shape[0]
    length = blocks * 128
    tiles = length // STEP
    lane = lax.broadcasted_iota(jnp.int32, (64, 128), 1)
    row = lax.broadcasted_iota(jnp.int32, (PART, STEP), 0)
    col = lax.broadcasted_iota(jnp.int32, (PART, STEP), 1)

    gates = -cum_ref[...]
    high = gates.astype(jnp.bfloat16).astype(jnp.float32)
    mid = (gates - high).astype(jnp.bfloat16).astype(jnp.float32)
    low = gates - high - mid
    blank = jnp.zeros((64, 128), jnp.float32)
    turned = jnp.concatenate([blank, high, mid, low, blank[:16]], axis=0).T.astype(jnp.bfloat16)
    queries_ref[64:112, :] = jnp.ones((48, length), jnp.bfloat16)
    queries_ref[112:, :] = jnp.zeros((16, length), jnp.bfloat16)
    values_ref[64:, :] = jnp.ones((16, length), jnp.bfloat16)
    nothing = jnp.zeros((64, 128), jnp.bfloat16)
    for p in range(blocks):
        spot = slice(p * 128, (p + 1) * 128)
        queries_ref[0:64, spot] = x_ref[p, 0:64, :]
        values_ref[0:64, spot] = x_ref[p, 64:128, :]
        both = x_ref[p, 128:192, :]
        other = jnp.concatenate([both[:, 64:], both[:, :64]], axis=1)
        for keys, part in ((both, 0), (other, 64)):
            gate = jnp.where((lane & 15) == p, turned[part : part + 64], nothing)
            keys_ref[p * 128 + part : p * 128 + part + 64, :] = jnp.where(lane < 64, keys, gate)

    def score(i, s, top):
        scores = jnp.dot(keys_ref[s : s + PART, :], queries_ref[:, i * STEP : (i + 1) * STEP], preferred_element_type=jnp.float32)
        if s >= i * STEP:
            scores = jnp.where(row + (s - i * STEP) <= col, scores, -jnp.inf)
        score_ref[i % 2, s : s + PART, :] = scores
        most = jnp.max(scores.reshape(PART // 8, 8, STEP), axis=0)
        return most if top is None else jnp.maximum(top, most)

    def weigh(i, s, top):
        expon_ref[i % 2, s : s + PART, :] = jnp.exp(score_ref[i % 2, s : s + PART, :] - top).astype(jnp.bfloat16)

    def finish(i):
        upto = (i + 1) * STEP
        both = jnp.dot(values_ref[:, :upto], expon_ref[i % 2, :upto, :], preferred_element_type=jnp.float32)
        head = (both[0:64] / both[64:65]).astype(jnp.bfloat16)
        out_ref[2 * i] = head[:, 0:128]
        out_ref[2 * i + 1] = head[:, 128:256]
        pair = pl.ds(2 * i, 2)
        copies.append(pltpu.make_async_copy(out_ref.at[pair], out_hbm.at[pair], sems.at[i]))
        copies[-1].start()

    copies = []
    tops = {}
    order = list(reversed(range(tiles)))
    for n, i in enumerate(order + [None]):
        before = order[n - 1] if n else None
        todo = list(range(0, (i + 1) * STEP, PART)) if i is not None else []
        late = list(range(0, (before + 1) * STEP, PART)) if n else []
        top = None
        for m in range(max(len(todo), len(late))):
            if m == min(2, max(len(todo), len(late)) - 1) and n > 1:
                finish(order[n - 2])
            if m < len(late):
                weigh(before, late[m], tops[before])
            if m < len(todo):
                top = score(i, todo[m], top)
        if top is not None:
            tops[i] = jnp.max(top, axis=0, keepdims=True)
    finish(order[-1])
    for copy in copies:
        copy.wait()


def attend(packed, cum):
    length = cum.size
    return pl.pallas_call(
        attend_kernel,
        out_shape=jax.ShapeDtypeStruct((16, 64, 128), jnp.bfloat16),
        in_specs=[VMEM] * 2,
        out_specs=HBM,
        scratch_shapes=[
            pltpu.VMEM((16, 64, 128), jnp.bfloat16),
            pltpu.SemaphoreType.DMA((8,)),
            pltpu.VMEM((length, 128), jnp.bfloat16),
            pltpu.VMEM((128, length), jnp.bfloat16),
            pltpu.VMEM((80, length), jnp.bfloat16),
            pltpu.VMEM((2, length, STEP), jnp.float32),
            pltpu.VMEM((2, length, STEP), jnp.bfloat16),
        ],
        compiler_params=pltpu.CompilerParams(vmem_limit_bytes=28 << 20),
    )(packed, cum)


def project_kernel(spot_ref, head_ref, *refs):
    *parts, out_hbm, turned_ref, out_ref, sems = refs
    y, x, core = spot_ref[0], spot_ref[1], spot_ref[2]
    heads = head_ref[...]
    for n, part in enumerate(parts):
        owner = core if n < 4 else 1 - core
        base = (((x + (0, -1, 1, 2)[n % 4] * (1 - 2 * owner)) & 3) * 2 + owner) * 32
        rows = jnp.dot(part[...], heads, preferred_element_type=jnp.float32)
        for m, back in enumerate((0, 4, 2, 6, 1, 5, 3, 7)):
            place = pl.multiple_of(((y - back) & 7) * 256 + base, 32)
            turned_ref[pl.ds(place, 32), :] = rows[m * 32 : (m + 1) * 32]
    copies = []
    for n in range(4):
        for m in range(4 * n, 4 * n + 4):
            cols = slice(m * 128, (m + 1) * 128)
            out_ref[:, cols] = turned_ref[cols, :].astype(jnp.bfloat16).T
        cols = slice(n * 512, (n + 1) * 512)
        copies.append(pltpu.make_async_copy(out_ref.at[:, cols], out_hbm.at[0, :, cols], sems.at[n]))
        copies[-1].start()
    for copy in copies:
        copy.wait()


def project(heads, parts):
    spot = jnp.stack([lax.axis_index(axis) for axis in DP])
    return pl.pallas_call(
        project_kernel,
        out_shape=jax.ShapeDtypeStruct((1, 128, 2048), jnp.bfloat16),
        in_specs=[pl.BlockSpec(memory_space=pltpu.SMEM)] + [VMEM] * (1 + len(parts)),
        out_specs=HBM,
        scratch_shapes=[
            pltpu.VMEM((2048, 128), jnp.float32),
            pltpu.VMEM((128, 2048), jnp.bfloat16),
            pltpu.SemaphoreType.DMA((4,)),
        ],
        compiler_params=pltpu.CompilerParams(vmem_limit_bytes=12 << 20),
    )(spot, heads, *parts)


def shift(value, axis, by):
    n = lax.axis_size(axis)
    return lax.ppermute(value, axis, [(s, (s + by) % n) for s in range(n)])


def gather_weight(out_weight):
    rows = out_weight.T
    for by in (4, 2, 1):
        rows = jnp.concatenate([rows, shift(rows, "dp_0", by)])
    there = [(i * 2 + c, (i + 1 - 2 * c) % 4 * 2 + c) for i in range(4) for c in range(2)]
    back = [(target, source) for source, target in there]
    near = [lax.ppermute(rows, DP[1:], way) for way in (there, back)]
    far = lax.ppermute(near[0], DP[1:], there)
    pieces = [rows, *near, far]
    others = [shift(rows, "dp_2", 1)]
    others += [shift(piece, "dp_2", 1) for piece in pieces[1:]]
    return pieces + others


def shards(queries, keys, values, cum_gates, out_weight):
    packed = pack(queries, keys, values)
    packed = lax.all_to_all(packed, "sp", split_axis=0, concat_axis=0, tiled=True)
    parts = gather_weight(out_weight)
    heads = attend(packed, cum_gates.reshape(16, 128))
    heads = lax.all_to_all(heads, "sp", split_axis=0, concat_axis=0, tiled=True)
    return project(heads.reshape(1024, 128), parts)


def solution(mesh):
    split = Mesh(mesh.devices.reshape(mesh.shape["sp"], 8, 4, 2), ("sp", "dp_0", "dp_1", "dp_2"))
    placed = (
        P(DP, "sp", None),
        P(DP, "sp", None),
        P(DP, "sp", None),
        P(DP, "sp", None),
        P(None, DP),
    )
    return jax.shard_map(
        shards, mesh=split, in_specs=placed, out_specs=P(DP, "sp", None), check_vma=False
    )
```
